32 devices in a mesh: fs: 16 (over z, y, core), tp: 2 (over x).
Axes of the slice: x: 2, y: 2, z: 4, core: 2. Of those that a mesh axis runs over, the one named last changes fastest.
Arguments:
- tokens: bfloat16 [8192, 2048], P('fs', 'tp'), may hold values from -6 to 6
- norm_gain: float32 [2048], P('fs'), may hold values from 0.1 to 1.9
- up_trained: float32 [2048, 4096], P('fs', 'tp'), may hold values from -0.125 to 0.125
- down_trained: float32 [4096, 2048], P('fs', 'tp'), may hold values from -0.09375 to 0.09375
Outputs:
- up_serving: bfloat16 [2048, 4096], P(None, 'tp')
- down_serving: bfloat16 [4096, 2048], P('tp')
- mixed: bfloat16 [8192, 2048], P('fs', 'tp')
The draws below stay inside these ranges and needn't reach their ends.
All inputs are finite; a program needn't handle non-finite values.
Results may differ from the reference program's by a relative error of at most 0.013.
Values may be sent and summed in bfloat16 or wider, within the bound.
A program may use at most 128 MiB of HBM per device.

```python
import jax
import jax.numpy as jnp
from jax import lax

D = 2048
FF = 4096
TOKENS = 8192
N_TP = 2


def shard_levels(rng, dims, shards, least, largest):
    def one(axis_at, parts):
        steps = jax.random.uniform(jax.random.fold_in(jax.random.fold_in(rng, 6), axis_at), (parts,), jnp.float32, least / len(shards), largest / len(shards))
        return jnp.repeat(jnp.exp(steps), dims[axis_at] // parts).reshape((-1,) + (1,) * (len(dims) - axis_at - 1))

    loudness = one(*shards[0])
    for cut in shards[1:]:
        loudness = loudness * one(*cut)
    return loudness


def centred(own_key, dims, width, limit, cuts=(), dtype=jnp.bfloat16):
    loudness = shard_levels(own_key, dims, cuts, -0.22, 0.18) if cuts else 1.0
    array = jax.random.normal(own_key, dims, jnp.float32) * width * loudness
    return jnp.minimum(jnp.maximum(array, -limit), limit).astype(dtype)


def setup_inputs(seed: int = 0) -> dict:
    keys = jax.random.split(jax.random.key(seed), 5)
    tokens = centred(keys[0], (TOKENS, D), 1.0, 6.0, ((0, 16), (1, 2)))
    norm_gain = jnp.clip(1.0 + 0.18 * jax.random.normal(keys[1], (D,), jnp.float32), 0.1, 1.9)
    up_trained = centred(keys[2], (D, FF), D ** -0.5, 0.125, ((0, 16), (1, 2)), jnp.float32)
    down_trained = centred(keys[3], (FF, D), FF ** -0.5, 0.09375, ((0, 16), (1, 2)), jnp.float32)
    return {"tokens": tokens, "norm_gain": norm_gain, "up_trained": up_trained, "down_trained": down_trained}


def reference(tokens, norm_gain, up_trained, down_trained):
    up_serving = (norm_gain[:, None] * up_trained).astype(jnp.bfloat16)
    down_serving = down_trained.astype(jnp.bfloat16)
    widened = tokens.astype(jnp.float32)
    scale = lax.rsqrt(lax.optimization_barrier(jnp.mean(widened * widened, axis=-1, keepdims=True)) + 1e-06)
    normed = (widened * scale).astype(jnp.bfloat16)
    preact = jnp.dot(normed, up_serving, preferred_element_type=jnp.float32)
    hidden = jnp.square(jnp.maximum(preact, 0.0)).astype(jnp.bfloat16)
    block = FF // N_TP
    mixed = jnp.zeros((tokens.shape[0], D), jnp.float32)
    for index in range(N_TP):
        part = jnp.dot(hidden[:, index * block:(index + 1) * block], down_serving[index * block:(index + 1) * block], preferred_element_type=jnp.float32)
        rounded = lax.optimization_barrier(part.astype(jnp.bfloat16))
        mixed = mixed + rounded.astype(jnp.float32)
    return (up_serving, down_serving, mixed.astype(jnp.bfloat16))
```

```python
import functools

import jax
import jax.numpy as jnp
from jax import lax
from jax.experimental import pallas as pl
from jax.experimental.pallas import tpu as pltpu
from jax.sharding import PartitionSpec as P

BF = jnp.bfloat16
F32 = jnp.float32


def plain_device(tokens, norm_gain, up_trained, down_trained):
    up_piece = (norm_gain[:, None] * up_trained).astype(BF)
    up_serving = lax.all_gather(up_piece, "fs", axis=0, tiled=True)
    down_piece = down_trained.astype(BF)
    group_count = lax.axis_size("fs")
    pair_count = lax.axis_size("tp")
    sliver = down_piece.shape[1] // group_count
    flipped = down_piece.T
    narrow = lax.all_to_all(flipped, "fs", split_axis=0, concat_axis=1, tiled=True)
    regrouped = lax.all_to_all(narrow, "tp", split_axis=1, concat_axis=0, tiled=True)
    spread = lax.all_gather(regrouped, "fs", axis=0, tiled=True)
    block_width = spread.shape[1]
    ordered = spread.reshape(group_count, pair_count, sliver, block_width).transpose(1, 0, 2, 3)
    down_serving = ordered.reshape(pair_count * group_count * sliver, block_width).T
    features = lax.all_gather(tokens, "tp", axis=1, tiled=True)
    widened = features.astype(F32)
    scale = lax.rsqrt(jnp.mean(widened * widened, axis=-1, keepdims=True) + 1e-06)
    normed = (widened * scale).astype(BF)
    preact = jnp.dot(normed, up_serving, preferred_element_type=F32)
    hidden = jnp.square(jnp.maximum(preact, 0.0)).astype(BF)
    partial_out = jnp.dot(hidden, down_serving, preferred_element_type=F32)
    summed = lax.psum_scatter(partial_out.astype(BF), "tp", scatter_dimension=1, tiled=True)
    return (up_serving, down_serving, summed)


def grid_of(mesh):
    n_fs, n_tp = mesh.shape["fs"], mesh.shape["tp"]
    if n_tp != 2 or n_fs % 4:
        return None
    ny, nc = 2, 2
    nz = n_fs // (ny * nc)
    if nz % n_tp:
        return None
    base = mesh.devices[0, 0].coords
    for f in range(n_fs):
        for t in range(n_tp):
            d = mesh.devices[f, t]
            at = (t, (f // nc) % ny, f // (nc * ny))
            if tuple(a - b for a, b in zip(d.coords, base)) != at or d.core_on_chip != f % nc:
                return None
    return nz, ny


def kernel(nz, tok_ref, upp_ref, dnp_ref, up_out, dn_out, mix_ref,
           up, dn, tok_peer, normed, hidden, part_out, part_in,
           up_recv, dn_recv, up_send, dn_send, x_send, x_recv, out_sem):
    f = lax.axis_index("fs")
    x = lax.axis_index("tp")
    c = f % 2
    y = (f // 2) % 2
    z = f // 4
    zb = nz // 2
    ru = upp_ref.shape[0]
    rd = dnp_ref.shape[0]
    rows, half = tok_ref.shape
    width = up.shape[1]
    local_f = f - x * (2 * zb * 2)
    in_block = (z // zb) == x

    def fs_of(zz, yy, cc):
        return (zz * 2 + yy) * 2 + cc

    right = {"fs": fs_of(z + 1, y, c)}
    left = {"fs": fs_of(z - 1, y, c)}
    across = {"fs": fs_of(z, 1 - y, c)}
    partner = {"fs": fs_of(z, y, 1 - c)}
    peer = {"tp": 1 - x}
    dirs = {"r": (0, right, z + 1 < nz), "l": (1, left, z > 0), "y": (2, across, None), "p": (3, partner, None)}

    barrier = pltpu.get_barrier_semaphore()

    def greet(who):
        pl.semaphore_signal(barrier, inc=1, device_id=who, device_id_type=pl.DeviceIdType.MESH)

    for who in (across, partner, peer):
        greet(who)
    pl.when(z + 1 < nz)(lambda: greet(right))
    pl.when(z > 0)(lambda: greet(left))
    pl.semaphore_wait(barrier, 3 + (z + 1 < nz).astype(jnp.int32) + (z > 0).astype(jnp.int32))

    sends = []

    def both(a, b):
        if a is None:
            return b
        if b is None:
            return a
        return jnp.logical_and(a, b)

    def guarded(cond, fn):
        if cond is None:
            fn()
        else:
            pl.when(cond)(fn)

    def rcopy(src, dst, ssem, rsem, who):
        return pltpu.make_async_remote_copy(src_ref=src, dst_ref=dst, send_sem=ssem, recv_sem=rsem,
                                            device_id=who, device_id_type=pl.DeviceIdType.MESH)

    def send(cond, make):
        guarded(cond, lambda: make().start())
        sends.append((cond, make))

    def up_slot(p):
        return up.at[pl.ds(pl.multiple_of(p * ru, ru), ru)]

    def dn_slot(h, q):
        return dn.at[h, pl.ds(pl.multiple_of(q * rd, rd), rd)]

    def up_forward(p, names, cond=None, src=None):
        for name in names:
            k, who, there = dirs[name]
            send(both(cond, there),
                 lambda k=k, who=who: rcopy(up_slot(p) if src is None else src, up_slot(p),
                                            up_send.at[p * 4 + k], up_recv.at[p], who))

    def up_wait(p, cond=None):
        guarded(cond, lambda: rcopy(up_slot(p), up_slot(p), up_send.at[p * 4], up_recv.at[p], partner).wait_recv())

    def sides(s):
        if s == 0:
            return [(z, None, None)]
        return [(z - s, z - s >= 0, "r"), (z + s, z + s < nz, "l")]

    def up_z(s):
        for zz, cond, onward in sides(s):
            p = fs_of(zz, y, c)
            up_wait(p, cond)
            up_forward(p, (onward, "y", "p"), cond)

    def up_y(s):
        for zz, cond, _ in sides(s):
            p = fs_of(zz, 1 - y, c)
            up_wait(p, cond)
            up_forward(p, ("p",), cond)

    def up_p(s):
        for zz, cond, _ in sides(s):
            for yy in (y, 1 - y):
                up_wait(fs_of(zz, yy, 1 - c), cond)

    def dn_id(zz, yy, cc):
        return fs_of(zz - x * zb, yy, cc)

    def dn_cond(zz, cond):
        return both(cond, (zz // zb) == x)

    def dn_forward(h, q, names, cond, src=None):
        for name in names:
            k, who, there = dirs[name]
            send(both(cond, there),
                 lambda k=k, who=who: rcopy(dn_slot(h, q) if src is None else src, dn_slot(h, q),
                                            dn_send.at[h, q * 4 + k], dn_recv.at[h, q], who))

    def dn_wait(h, q, cond):
        guarded(cond, lambda: rcopy(dn_slot(h, q), dn_slot(h, q), dn_send.at[h, q * 4], dn_recv.at[h, q],
                                    partner).wait_recv())

    def dn_src(h):
        if h == 0:
            dn_wait(0, local_f, in_block)
            dn_forward(0, local_f, ("r", "l", "y", "p"), in_block)
        else:
            dn_forward(1, local_f, ("r", "l", "y", "p"), in_block, src=dnp_ref)

    def dn_z(h, s):
        for zz, cond, onward in sides(s):
            cond = dn_cond(zz, cond)
            q = dn_id(zz, y, c)
            dn_wait(h, q, cond)
            dn_forward(h, q, (onward, "y", "p"), cond)

    def dn_y(h, s):
        for zz, cond, _ in sides(s):
            cond = dn_cond(zz, cond)
            q = dn_id(zz, 1 - y, c)
            dn_wait(h, q, cond)
            dn_forward(h, q, ("p",), cond)

    def dn_p(h, s):
        for zz, cond, _ in sides(s):
            cond = dn_cond(zz, cond)
            for yy in (y, 1 - y):
                dn_wait(h, dn_id(zz, yy, 1 - c), cond)

    def tile(i, n):
        return pl.ds(pl.multiple_of(i * n, n), n)

    nt = min(256, half, width)
    rt = min(64, rows)
    reps = width // nt

    def norm():
        @pl.loop(0, rows // rt)
        def _(i):
            r = tile(i, rt)
            mine = tok_ref[r, :].astype(F32)
            other = tok_peer[r, :].astype(F32)
            total = jnp.sum(mine * mine, axis=-1, keepdims=True) + jnp.sum(other * other, axis=-1, keepdims=True)
            scale = lax.rsqrt(total / (2 * half) + 1e-06)
            normed[x, r, :] = (mine * scale).astype(BF)
            normed[1 - x, r, :] = (other * scale).astype(BF)

    def up_dot(lo, hi):
        @pl.loop(lo, hi)
        def _(i):
            cols = tile(i, nt)
            acc = jnp.dot(normed[0], up[pl.ds(0, half), cols], preferred_element_type=F32)
            acc = acc + jnp.dot(normed[1], up[pl.ds(half, half), cols], preferred_element_type=F32)
            hidden[:, cols] = jnp.square(jnp.maximum(acc, 0.0)).astype(BF)

    def dn_dot(h, dst, extra=None):
        @pl.loop(0, half // nt)
        def _(i):
            cols = tile(i, nt)
            acc = jnp.dot(hidden[...], dn[h, :, cols], preferred_element_type=F32).astype(BF)
            if extra is not None:
                acc = (acc.astype(F32) + extra[:, cols].astype(F32)).astype(BF)
            dst[:, cols] = acc

    cross = lambda: rcopy(dnp_ref, dn_slot(0, f - (1 - x) * (2 * zb * 2)), x_send.at[0],
                          dn_recv.at[0, f - (1 - x) * (2 * zb * 2)], peer)
    send(jnp.logical_not(in_block), cross)
    send_tok = lambda: rcopy(tok_ref, tok_peer, x_send.at[1], x_recv.at[0], peer)
    send(None, send_tok)
    up_forward(f, ("r", "l", "y", "p"), src=upp_ref)
    own_up = pltpu.make_async_copy(upp_ref, up_slot(f), out_sem.at[0])
    own_up.start()
    own_dn = lambda: pltpu.make_async_copy(dnp_ref, dn_slot(1, local_f), out_sem.at[1])
    pl.when(in_block)(lambda: own_dn().start())

    last = nz - 1
    up_z(1)
    dn_src(0)
    up_y(0)
    for s in range(2, nz):
        up_z(s)
        dn_z(0, s - 1)
    up_y(1)
    dn_src(1)
    for s in range(2, nz):
        up_y(s)
    dn_z(0, last)
    send_tok().wait_recv()
    norm()
    own_up.wait()
    for s in range(nz):
        up_p(s)
    up_store = pltpu.make_async_copy(up, up_out, out_sem.at[2])
    up_store.start()
    dn_y(0, 0)
    cuts = [reps * k // nz for k in range(nz + 1)]
    for s in range(nz):
        up_dot(cuts[s], cuts[s + 1])
        if s + 1 < nz:
            dn_z(1, s + 1)
            dn_y(0, s + 1)
    for s in range(nz):
        dn_p(0, s)

    def store_half(h, sem):
        off = (1 - x if h == 0 else x) * half
        return pltpu.make_async_copy(dn.at[h], dn_out.at[:, pl.ds(pl.multiple_of(off, half), half)], sem)

    dn_dot(0, part_out)
    store_half(0, out_sem.at[3]).start()
    dn_y(1, 0)
    send_part = lambda: rcopy(part_out, part_in, x_send.at[2], x_recv.at[1], peer)
    send(None, send_part)
    for s in range(1, nz):
        dn_y(1, s)
    pl.when(in_block)(lambda: own_dn().wait())
    for s in range(nz):
        dn_p(1, s)
    store_half(1, out_sem.at[4]).start()
    send_part().wait_recv()
    dn_dot(1, mix_ref, part_in)
    for cond, make in sends:
        guarded(cond, lambda make=make: make().wait_send())
    up_store.wait()
    store_half(0, out_sem.at[3]).wait()
    store_half(1, out_sem.at[4]).wait()


def grid_device(nz, tokens, norm_gain, up_trained, down_trained):
    up_piece = (norm_gain[:, None] * up_trained).astype(BF)
    down_piece = down_trained.astype(BF)
    n_fs, n_tp = lax.axis_size("fs"), lax.axis_size("tp")
    ru, width = up_piece.shape
    rd, half = down_piece.shape
    rows = tokens.shape[0]
    d_model, blk = ru * n_fs, n_fs // n_tp
    vmem = pl.BlockSpec(memory_space=pltpu.VMEM)
    hbm = pl.BlockSpec(memory_space=pl.ANY)
    flops = 2 * rows * width * d_model * 2
    return pl.pallas_call(
        functools.partial(kernel, nz),
        out_shape=(
            jax.ShapeDtypeStruct((d_model, width), BF),
            jax.ShapeDtypeStruct((rd * blk, half * n_tp), BF),
            jax.ShapeDtypeStruct((rows, half), BF),
        ),
        in_specs=[vmem, vmem, vmem],
        out_specs=(hbm, hbm, vmem),
        scratch_shapes=[
            pltpu.VMEM((d_model, width), BF),
            pltpu.VMEM((n_tp, rd * blk, half), BF),
            pltpu.VMEM((rows, half), BF),
            pltpu.VMEM((n_tp, rows, half), BF),
            pltpu.VMEM((rows, width), BF),
            pltpu.VMEM((rows, half), BF),
            pltpu.VMEM((rows, half), BF),
            pltpu.SemaphoreType.DMA((n_fs,)),
            pltpu.SemaphoreType.DMA((n_tp, blk)),
            pltpu.SemaphoreType.DMA((n_fs * 4,)),
            pltpu.SemaphoreType.DMA((n_tp, blk * 4)),
            pltpu.SemaphoreType.DMA((3,)),
            pltpu.SemaphoreType.DMA((2,)),
            pltpu.SemaphoreType.DMA((5,)),
        ],
        compiler_params=pltpu.CompilerParams(
            collective_id=0, has_side_effects=True, vmem_limit_bytes=56 * 2**20
        ),
        cost_estimate=pl.CostEstimate(flops=flops, bytes_accessed=2 * d_model * width * 2, transcendentals=0),
    )(tokens, up_piece, down_piece)


def solution(mesh):
    placed = (P("fs", "tp"), P("fs"), P("fs", "tp"), P("fs", "tp"))
    grid = grid_of(mesh)
    body = plain_device if grid is None else functools.partial(grid_device, grid[0])
    return jax.shard_map(
        body,
        mesh=mesh,
        in_specs=placed,
        out_specs=(P(None, "tp"), P("tp", None), P("fs", "tp")),
        check_vma=False,
    )
```

```python
import functools

import jax
import jax.numpy as jnp
from jax import lax
from jax.experimental import pallas as pl
from jax.experimental.pallas import tpu as pltpu
from jax.sharding import PartitionSpec as P

BF = jnp.bfloat16
F32 = jnp.float32


def plain_device(tokens, norm_gain, up_trained, down_trained):
    up_piece = (norm_gain[:, None] * up_trained).astype(BF)
    up_serving = lax.all_gather(up_piece, "fs", axis=0, tiled=True)
    down_piece = down_trained.astype(BF)
    group_count = lax.axis_size("fs")
    pair_count = lax.axis_size("tp")
    sliver = down_piece.shape[1] // group_count
    flipped = down_piece.T
    narrow = lax.all_to_all(flipped, "fs", split_axis=0, concat_axis=1, tiled=True)
    regrouped = lax.all_to_all(narrow, "tp", split_axis=1, concat_axis=0, tiled=True)
    spread = lax.all_gather(regrouped, "fs", axis=0, tiled=True)
    block_width = spread.shape[1]
    ordered = spread.reshape(group_count, pair_count, sliver, block_width).transpose(1, 0, 2, 3)
    down_serving = ordered.reshape(pair_count * group_count * sliver, block_width).T
    features = lax.all_gather(tokens, "tp", axis=1, tiled=True)
    widened = features.astype(F32)
    scale = lax.rsqrt(jnp.mean(widened * widened, axis=-1, keepdims=True) + 1e-06)
    normed = (widened * scale).astype(BF)
    preact = jnp.dot(normed, up_serving, preferred_element_type=F32)
    hidden = jnp.square(jnp.maximum(preact, 0.0)).astype(BF)
    partial_out = jnp.dot(hidden, down_serving, preferred_element_type=F32)
    summed = lax.psum_scatter(partial_out.astype(BF), "tp", scatter_dimension=1, tiled=True)
    return (up_serving, down_serving, summed)


def grid_of(mesh):
    n_fs, n_tp = mesh.shape["fs"], mesh.shape["tp"]
    if n_tp != 2 or n_fs % 4:
        return None
    ny, nc = 2, 2
    nz = n_fs // (ny * nc)
    if nz % n_tp:
        return None
    base = mesh.devices[0, 0].coords
    for f in range(n_fs):
        for t in range(n_tp):
            d = mesh.devices[f, t]
            at = (t, (f // nc) % ny, f // (nc * ny))
            if tuple(a - b for a, b in zip(d.coords, base)) != at or d.core_on_chip != f % nc:
                return None
    return nz, ny


PARTS = 2


def kernel(nz, tok_ref, gain_ref, upt_ref, dnt_ref, up, dn, hidden, part_in,
           dnp_ref, tok_peer, normed, part_out,
           up_recv, dn_recv, up_send, dn_send, x_send, x_recv, out_sem):
    f = lax.axis_index("fs")
    x = lax.axis_index("tp")
    c = f % 2
    y = (f // 2) % 2
    z = f // 4
    zb = nz // 2
    ru = upt_ref.shape[0]
    rd = dnp_ref.shape[0]
    su, sd = ru // PARTS, rd // PARTS
    rows, half = tok_ref.shape
    width = up.shape[1]
    local_f = f - x * (2 * zb * 2)
    in_block = (z // zb) == x

    def fs_of(zz, yy, cc):
        return (zz * 2 + yy) * 2 + cc

    right = {"fs": fs_of(z + 1, y, c)}
    left = {"fs": fs_of(z - 1, y, c)}
    across = {"fs": fs_of(z, 1 - y, c)}
    partner = {"fs": fs_of(z, y, 1 - c)}
    peer = {"tp": 1 - x}
    dirs = {"r": (0, right, z + 1 < nz), "l": (1, left, z > 0), "y": (2, across, None), "p": (3, partner, None)}

    lanes = 128
    spread = jnp.broadcast_to(gain_ref[...], (lanes, ru)).T

    @pl.loop(0, width // lanes)
    def _(i):
        cols = pl.ds(pl.multiple_of(i * lanes, lanes), lanes)
        up[pl.ds(pl.multiple_of(f * ru, ru), ru), cols] = (spread * upt_ref[:, cols]).astype(BF)

    @pl.loop(0, rd // 32)
    def _(i):
        r = pl.ds(pl.multiple_of(i * 32, 32), 32)
        dnp_ref[r, :] = dnt_ref[r, :].astype(BF)

    barrier = pltpu.get_barrier_semaphore()

    def greet(who):
        pl.semaphore_signal(barrier, inc=1, device_id=who, device_id_type=pl.DeviceIdType.MESH)

    for who in (across, partner, peer):
        greet(who)
    pl.when(z + 1 < nz)(lambda: greet(right))
    pl.when(z > 0)(lambda: greet(left))
    pl.semaphore_wait(barrier, 3 + (z + 1 < nz).astype(jnp.int32) + (z > 0).astype(jnp.int32))

    sends = []

    def both(a, b):
        if a is None:
            return b
        if b is None:
            return a
        return jnp.logical_and(a, b)

    def guarded(cond, fn):
        if cond is None:
            fn()
        else:
            pl.when(cond)(fn)

    def rcopy(src, dst, ssem, rsem, who):
        return pltpu.make_async_remote_copy(src_ref=src, dst_ref=dst, send_sem=ssem, recv_sem=rsem,
                                            device_id=who, device_id_type=pl.DeviceIdType.MESH)

    def send(cond, make):
        guarded(cond, lambda: make().start())
        sends.append((cond, make))

    def up_slot(p, k):
        return up.at[pl.ds(pl.multiple_of(p * ru + k * su, su), su)]

    def dn_slot(h, q, k):
        return dn.at[h, pl.ds(pl.multiple_of(q * rd + k * sd, sd), sd)]

    def dnp(k):
        return dnp_ref.at[pl.ds(k * sd, sd)]

    def up_forward(p, k, names, cond=None):
        for name in names:
            j, who, there = dirs[name]
            send(both(cond, there),
                 lambda j=j, who=who: rcopy(up_slot(p, k), up_slot(p, k), up_send.at[k, p * 4 + j],
                                            up_recv.at[k, p], who))

    def up_wait(p, k, cond=None):
        guarded(cond, lambda: rcopy(up_slot(p, k), up_slot(p, k), up_send.at[k, p * 4], up_recv.at[k, p],
                                    partner).wait_recv())

    def sides(s):
        if s == 0:
            return [(z, None, None)]
        return [(z - s, z - s >= 0, "r"), (z + s, z + s < nz, "l")]

    def each(s):
        return [(k, *side) for k in range(PARTS) for side in sides(s)]

    def up_z(s):
        for k, zz, cond, onward in each(s):
            p = fs_of(zz, y, c)
            up_wait(p, k, cond)
            up_forward(p, k, (onward, "y", "p"), cond)

    def up_y(s):
        for k, zz, cond, _ in each(s):
            p = fs_of(zz, 1 - y, c)
            up_wait(p, k, cond)
            up_forward(p, k, ("p",), cond)

    def up_p(s):
        for k, zz, cond, _ in each(s):
            for yy in (y, 1 - y):
                up_wait(fs_of(zz, yy, 1 - c), k, cond)

    def dn_id(zz, yy, cc):
        return fs_of(zz - x * zb, yy, cc)

    def dn_cond(zz, cond):
        return both(cond, (zz // zb) == x)

    def dn_forward(h, q, k, names, cond, src=None):
        for name in names:
            j, who, there = dirs[name]
            send(both(cond, there),
                 lambda j=j, who=who: rcopy(dn_slot(h, q, k) if src is None else src, dn_slot(h, q, k),
                                            dn_send.at[h, k, q * 4 + j], dn_recv.at[h, k, q], who))

    def dn_wait(h, q, k, cond):
        guarded(cond, lambda: rcopy(dn_slot(h, q, k), dn_slot(h, q, k), dn_send.at[h, k, q * 4],
                                    dn_recv.at[h, k, q], partner).wait_recv())

    def dn_src(h):
        for k in range(PARTS):
            if h == 0:
                dn_wait(0, local_f, k, in_block)
                dn_forward(0, local_f, k, ("r", "l", "y", "p"), in_block)
            else:
                dn_forward(1, local_f, k, ("r", "l", "y", "p"), in_block, src=dnp(k))

    def dn_z(h, s):
        for k, zz, cond, onward in each(s):
            cond = dn_cond(zz, cond)
            q = dn_id(zz, y, c)
            dn_wait(h, q, k, cond)
            dn_forward(h, q, k, (onward, "y", "p"), cond)

    def dn_y(h, s):
        for k, zz, cond, _ in each(s):
            cond = dn_cond(zz, cond)
            q = dn_id(zz, 1 - y, c)
            dn_wait(h, q, k, cond)
            dn_forward(h, q, k, ("p",), cond)

    def dn_p(h, s):
        for k, zz, cond, _ in each(s):
            cond = dn_cond(zz, cond)
            for yy in (y, 1 - y):
                dn_wait(h, dn_id(zz, yy, 1 - c), k, cond)

    def tile(i, n):
        return pl.ds(pl.multiple_of(i * n, n), n)

    nt = min(256, half, width)
    rt = min(64, rows)
    reps = width // nt

    def norm():
        @pl.loop(0, rows // rt)
        def _(i):
            r = tile(i, rt)
            mine = tok_ref[r, :].astype(F32)
            other = tok_peer[r, :].astype(F32)
            total = jnp.sum(mine * mine, axis=-1, keepdims=True) + jnp.sum(other * other, axis=-1, keepdims=True)
            scale = lax.rsqrt(total / (2 * half) + 1e-06)
            normed[x, r, :] = (mine * scale).astype(BF)
            normed[1 - x, r, :] = (other * scale).astype(BF)

    def up_dot(lo, hi):
        @pl.loop(lo, hi)
        def _(i):
            cols = tile(i, nt)
            acc = jnp.dot(normed[0], up[pl.ds(0, half), cols], preferred_element_type=F32)
            acc = acc + jnp.dot(normed[1], up[pl.ds(half, half), cols], preferred_element_type=F32)
            hidden[:, cols] = jnp.square(jnp.maximum(acc, 0.0)).astype(BF)

    def dn_dot(h, dst):
        @pl.loop(0, half // nt)
        def _(i):
            cols = tile(i, nt)
            dst[:, cols] = jnp.dot(hidden[...], dn[h, :, cols], preferred_element_type=F32).astype(BF)

    far_q = f - (1 - x) * (2 * zb * 2)
    for k in range(PARTS):
        send(jnp.logical_not(in_block),
             lambda k=k: rcopy(dnp(k), dn_slot(0, far_q, k), x_send.at[2 + k], dn_recv.at[0, k, far_q], peer))
    send_tok = lambda: rcopy(tok_ref, tok_peer, x_send.at[0], x_recv.at[0], peer)
    send(None, send_tok)
    for k in range(PARTS):
        up_forward(f, k, ("r", "l", "y", "p"))
    own_dn = lambda: pltpu.make_async_copy(dnp_ref, dn.at[1, pl.ds(pl.multiple_of(local_f * rd, rd), rd)],
                                           out_sem.at[0])
    pl.when(in_block)(lambda: own_dn().start())

    last = nz - 1
    up_z(1)
    dn_src(0)
    up_y(0)
    for s in range(2, nz):
        up_z(s)
        dn_z(0, s - 1)
    up_y(1)
    dn_src(1)
    for s in range(2, nz):
        up_y(s)
    dn_z(0, last)
    send_tok().wait_recv()
    norm()
    for s in range(nz):
        up_p(s)
    dn_y(0, 0)
    cuts = [reps * k // nz for k in range(nz + 1)]
    for s in range(nz):
        up_dot(cuts[s], cuts[s + 1])
        if s + 1 < nz:
            dn_z(1, s + 1)
            dn_y(0, s + 1)
    for s in range(nz):
        dn_p(0, s)

    dn_dot(0, part_out)
    dn_y(1, 0)
    send_part = lambda: rcopy(part_out, part_in, x_send.at[1], x_recv.at[1], peer)
    send(None, send_part)
    for s in range(1, nz):
        dn_y(1, s)
    pl.when(in_block)(lambda: own_dn().wait())
    for s in range(nz):
        dn_p(1, s)
    send_part().wait_recv()
    for cond, make in sends:
        guarded(cond, lambda make=make: make().wait_send())


def finish(up, dn, hidden, part_in, up_out, dn_out, mix_out, mix, sems):
    x = lax.axis_index("tp")
    half = dn.shape[2]
    n = sems.shape[1]
    ru, rd = up.shape[0] // n, dn.shape[1] // n
    off = [(1 - x) * half, x * half]
    copies = []
    for k in range(n):
        r = pl.ds(k * ru, ru)
        copies.append(pltpu.make_async_copy(up.at[r], up_out.at[r], sems.at[0, k]))
        r = pl.ds(k * rd, rd)
        for h in range(2):
            cols = pl.ds(pl.multiple_of(off[h], half), half)
            copies.append(pltpu.make_async_copy(dn.at[h, r], dn_out.at[r, cols], sems.at[1 + h, k]))
    for copy in copies:
        copy.start()
    nt = min(256, half)

    @pl.loop(0, half // nt)
    def _(i):
        cols = pl.ds(pl.multiple_of(i * nt, nt), nt)
        own = jnp.dot(hidden[...], dn[1, :, cols], preferred_element_type=F32).astype(BF)
        mix[:, cols] = (own.astype(F32) + part_in[:, cols].astype(F32)).astype(BF)

    last = pltpu.make_async_copy(mix, mix_out, sems.at[3, 0])
    last.start()
    for copy in copies:
        copy.wait()
    last.wait()


def grid_device(nz, tokens, norm_gain, up_trained, down_trained):
    n_fs, n_tp = lax.axis_size("fs"), lax.axis_size("tp")
    ru, width = up_trained.shape
    rd, half = down_trained.shape
    rows = tokens.shape[0]
    d_model, blk = ru * n_fs, n_fs // n_tp
    vmem = pl.BlockSpec(memory_space=pltpu.VMEM)
    hbm = pl.BlockSpec(memory_space=pl.ANY)
    flops = 2 * rows * width * d_model
    held = pl.pallas_call(
        functools.partial(kernel, nz),
        out_shape=(
            jax.ShapeDtypeStruct((d_model, width), BF),
            jax.ShapeDtypeStruct((n_tp, rd * blk, half), BF),
            jax.ShapeDtypeStruct((rows, width), BF),
            jax.ShapeDtypeStruct((rows, half), BF),
        ),
        in_specs=[vmem] * 4,
        out_specs=(vmem,) * 4,
        scratch_shapes=[
            pltpu.VMEM((rd, half), BF),
            pltpu.VMEM((rows, half), BF),
            pltpu.VMEM((n_tp, rows, half), BF),
            pltpu.VMEM((rows, half), BF),
            pltpu.SemaphoreType.DMA((PARTS, n_fs)),
            pltpu.SemaphoreType.DMA((n_tp, PARTS, blk)),
            pltpu.SemaphoreType.DMA((PARTS, n_fs * 4)),
            pltpu.SemaphoreType.DMA((n_tp, PARTS, blk * 4)),
            pltpu.SemaphoreType.DMA((2 + PARTS,)),
            pltpu.SemaphoreType.DMA((2,)),
            pltpu.SemaphoreType.DMA((1,)),
        ],
        compiler_params=pltpu.CompilerParams(
            collective_id=0, has_side_effects=True, vmem_limit_bytes=16 * 2**20
        ),
        cost_estimate=pl.CostEstimate(flops=flops, bytes_accessed=2 * d_model * width * 2, transcendentals=0),
    )(tokens, norm_gain.reshape(1, ru), up_trained, down_trained)
    return pl.pallas_call(
        finish,
        out_shape=(
            jax.ShapeDtypeStruct((d_model, width), BF),
            jax.ShapeDtypeStruct((rd * blk, half * n_tp), BF),
            jax.ShapeDtypeStruct((rows, half), BF),
        ),
        in_specs=[vmem] * 4,
        out_specs=(hbm,) * 3,
        scratch_shapes=[pltpu.VMEM((rows, half), BF), pltpu.SemaphoreType.DMA((4, 8))],
        compiler_params=pltpu.CompilerParams(vmem_limit_bytes=8 * 2**20),
        cost_estimate=pl.CostEstimate(flops=flops, bytes_accessed=2 * d_model * width * 2, transcendentals=0),
    )(*held)


def solution(mesh):
    placed = (P("fs", "tp"), P("fs"), P("fs", "tp"), P("fs", "tp"))
    grid = grid_of(mesh)
    body = plain_device if grid is None else functools.partial(grid_device, grid[0])
    return jax.shard_map(
        body,
        mesh=mesh,
        in_specs=placed,
        out_specs=(P(None, "tp"), P("tp", None), P("fs", "tp")),
        check_vma=False,
    )
```

```python
import functools

import jax
import jax.numpy as jnp
from jax import lax
from jax.experimental import pallas as pl
from jax.experimental.pallas import tpu as pltpu
from jax.sharding import PartitionSpec as P

BF = jnp.bfloat16
F32 = jnp.float32


def plain_device(tokens, norm_gain, up_trained, down_trained):
    up_piece = (norm_gain[:, None] * up_trained).astype(BF)
    up_serving = lax.all_gather(up_piece, "fs", axis=0, tiled=True)
    down_piece = down_trained.astype(BF)
    group_count = lax.axis_size("fs")
    pair_count = lax.axis_size("tp")
    sliver = down_piece.shape[1] // group_count
    flipped = down_piece.T
    narrow = lax.all_to_all(flipped, "fs", split_axis=0, concat_axis=1, tiled=True)
    regrouped = lax.all_to_all(narrow, "tp", split_axis=1, concat_axis=0, tiled=True)
    spread = lax.all_gather(regrouped, "fs", axis=0, tiled=True)
    block_width = spread.shape[1]
    ordered = spread.reshape(group_count, pair_count, sliver, block_width).transpose(1, 0, 2, 3)
    down_serving = ordered.reshape(pair_count * group_count * sliver, block_width).T
    features = lax.all_gather(tokens, "tp", axis=1, tiled=True)
    widened = features.astype(F32)
    scale = lax.rsqrt(jnp.mean(widened * widened, axis=-1, keepdims=True) + 1e-06)
    normed = (widened * scale).astype(BF)
    preact = jnp.dot(normed, up_serving, preferred_element_type=F32)
    hidden = jnp.square(jnp.maximum(preact, 0.0)).astype(BF)
    partial_out = jnp.dot(hidden, down_serving, preferred_element_type=F32)
    summed = lax.psum_scatter(partial_out.astype(BF), "tp", scatter_dimension=1, tiled=True)
    return (up_serving, down_serving, summed)


def grid_of(mesh):
    n_fs, n_tp = mesh.shape["fs"], mesh.shape["tp"]
    if n_tp != 2 or n_fs % 4:
        return None
    ny, nc = 2, 2
    nz = n_fs // (ny * nc)
    if nz % n_tp:
        return None
    base = mesh.devices[0, 0].coords
    for f in range(n_fs):
        for t in range(n_tp):
            d = mesh.devices[f, t]
            at = (t, (f // nc) % ny, f // (nc * ny))
            if tuple(a - b for a, b in zip(d.coords, base)) != at or d.core_on_chip != f % nc:
                return None
    return nz, ny


PARTS = 2


def kernel(nz, tok_ref, gain_ref, upt_ref, dnt_ref, up, dn, hidden, part_in,
           dnp_ref, tok_peer, normed, part_out,
           up_recv, dn_recv, up_send, dn_send, x_send, x_recv, out_sem):
    f = lax.axis_index("fs")
    x = lax.axis_index("tp")
    c = f % 2
    y = (f // 2) % 2
    z = f // 4
    zb = nz // 2
    ru = upt_ref.shape[0]
    rd = dnp_ref.shape[0]
    su, sd = ru // PARTS, rd // PARTS
    rows, half = tok_ref.shape
    width = up.shape[1]
    local_f = f - x * (2 * zb * 2)
    in_block = (z // zb) == x

    def fs_of(zz, yy, cc):
        return (zz * 2 + yy) * 2 + cc

    right = {"fs": fs_of(z + 1, y, c)}
    left = {"fs": fs_of(z - 1, y, c)}
    across = {"fs": fs_of(z, 1 - y, c)}
    partner = {"fs": fs_of(z, y, 1 - c)}
    peer = {"tp": 1 - x}
    dirs = {"r": (0, right, z + 1 < nz), "l": (1, left, z > 0), "y": (2, across, None), "p": (3, partner, None)}

    lanes = 128
    spread = jnp.broadcast_to(gain_ref[...], (lanes, ru)).T

    @pl.loop(0, width // lanes)
    def _(i):
        cols = pl.ds(pl.multiple_of(i * lanes, lanes), lanes)
        up[pl.ds(pl.multiple_of(f * ru, ru), ru), cols] = (spread * upt_ref[:, cols]).astype(BF)

    @pl.loop(0, rd // 32)
    def _(i):
        r = pl.ds(pl.multiple_of(i * 32, 32), 32)
        dnp_ref[r, :] = dnt_ref[r, :].astype(BF)

    barrier = pltpu.get_barrier_semaphore()

    def greet(who):
        pl.semaphore_signal(barrier, inc=1, device_id=who, device_id_type=pl.DeviceIdType.MESH)

    for who in (across, partner, peer):
        greet(who)
    pl.when(z + 1 < nz)(lambda: greet(right))
    pl.when(z > 0)(lambda: greet(left))
    pl.semaphore_wait(barrier, 3 + (z + 1 < nz).astype(jnp.int32) + (z > 0).astype(jnp.int32))

    sends = []

    def both(a, b):
        if a is None:
            return b
        if b is None:
            return a
        return jnp.logical_and(a, b)

    def guarded(cond, fn):
        if cond is None:
            fn()
        else:
            pl.when(cond)(fn)

    def rcopy(src, dst, ssem, rsem, who):
        return pltpu.make_async_remote_copy(src_ref=src, dst_ref=dst, send_sem=ssem, recv_sem=rsem,
                                            device_id=who, device_id_type=pl.DeviceIdType.MESH)

    def send(cond, make):
        guarded(cond, lambda: make().start())
        sends.append((cond, make))

    def up_slot(p, k):
        return up.at[pl.ds(pl.multiple_of(p * ru + k * su, su), su)]

    def dn_slot(h, q, k):
        return dn.at[h, pl.ds(pl.multiple_of(q * rd + k * sd, sd), sd)]

    def dnp(k):
        return dnp_ref.at[pl.ds(k * sd, sd)]

    def up_forward(p, k, names, cond=None):
        for name in names:
            j, who, there = dirs[name]
            send(both(cond, there),
                 lambda j=j, who=who: rcopy(up_slot(p, k), up_slot(p, k), up_send.at[k, p * 4 + j],
                                            up_recv.at[k, p], who))

    def up_wait(p, k, cond=None):
        guarded(cond, lambda: rcopy(up_slot(p, k), up_slot(p, k), up_send.at[k, p * 4], up_recv.at[k, p],
                                    partner).wait_recv())

    def sides(s):
        if s == 0:
            return [(z, None, None)]
        return [(z - s, z - s >= 0, "r"), (z + s, z + s < nz, "l")]

    def each(s):
        return [(k, *side) for k in range(PARTS) for side in sides(s)]

    def up_z(s):
        for k, zz, cond, onward in each(s):
            p = fs_of(zz, y, c)
            up_wait(p, k, cond)
            up_forward(p, k, (onward, "y", "p"), cond)

    def up_y(s):
        for k, zz, cond, _ in each(s):
            p = fs_of(zz, 1 - y, c)
            up_wait(p, k, cond)
            up_forward(p, k, ("p",), cond)

    def up_p(s):
        for k, zz, cond, _ in each(s):
            for yy in (y, 1 - y):
                up_wait(fs_of(zz, yy, 1 - c), k, cond)

    def dn_id(zz, yy, cc):
        return fs_of(zz - x * zb, yy, cc)

    def dn_cond(zz, cond):
        return both(cond, (zz // zb) == x)

    def dn_forward(h, q, k, names, cond, src=None):
        for name in names:
            j, who, there = dirs[name]
            send(both(cond, there),
                 lambda j=j, who=who: rcopy(dn_slot(h, q, k) if src is None else src, dn_slot(h, q, k),
                                            dn_send.at[h, k, q * 4 + j], dn_recv.at[h, k, q], who))

    def dn_wait(h, q, k, cond):
        guarded(cond, lambda: rcopy(dn_slot(h, q, k), dn_slot(h, q, k), dn_send.at[h, k, q * 4],
                                    dn_recv.at[h, k, q], partner).wait_recv())

    def dn_src(h):
        for k in range(PARTS):
            if h == 0:
                dn_wait(0, local_f, k, in_block)
                dn_forward(0, local_f, k, ("r", "l", "y", "p"), in_block)
            else:
                dn_forward(1, local_f, k, ("r", "l", "y", "p"), in_block, src=dnp(k))

    def dn_z(h, s):
        for k, zz, cond, onward in each(s):
            cond = dn_cond(zz, cond)
            q = dn_id(zz, y, c)
            dn_wait(h, q, k, cond)
            dn_forward(h, q, k, (onward, "y", "p"), cond)

    def dn_y(h, s):
        for k, zz, cond, _ in each(s):
            cond = dn_cond(zz, cond)
            q = dn_id(zz, 1 - y, c)
            dn_wait(h, q, k, cond)
            dn_forward(h, q, k, ("p",), cond)

    def dn_p(h, s):
        for k, zz, cond, _ in each(s):
            cond = dn_cond(zz, cond)
            for yy in (y, 1 - y):
                dn_wait(h, dn_id(zz, yy, 1 - c), k, cond)

    def tile(i, n):
        return pl.ds(pl.multiple_of(i * n, n), n)

    nt = min(256, half, width)
    rt = min(64, rows)
    reps = width // nt

    def norm():
        @pl.loop(0, rows // rt)
        def _(i):
            r = tile(i, rt)
            mine = tok_ref[r, :].astype(F32)
            other = tok_peer[r, :].astype(F32)
            total = jnp.sum(mine * mine, axis=-1, keepdims=True) + jnp.sum(other * other, axis=-1, keepdims=True)
            scale = lax.rsqrt(total / (2 * half) + 1e-06)
            normed[x, r, :] = (mine * scale).astype(BF)
            normed[1 - x, r, :] = (other * scale).astype(BF)

    def up_dot(lo, hi):
        @pl.loop(lo, hi)
        def _(i):
            cols = tile(i, nt)
            acc = jnp.dot(normed[0], up[pl.ds(0, half), cols], preferred_element_type=F32)
            acc = acc + jnp.dot(normed[1], up[pl.ds(half, half), cols], preferred_element_type=F32)
            hidden[:, cols] = jnp.square(jnp.maximum(acc, 0.0)).astype(BF)

    def dn_dot(h, dst):
        @pl.loop(0, half // nt)
        def _(i):
            cols = tile(i, nt)
            dst[:, cols] = jnp.dot(hidden[...], dn[h, :, cols], preferred_element_type=F32).astype(BF)

    far_q = f - (1 - x) * (2 * zb * 2)
    for k in range(PARTS):
        send(jnp.logical_not(in_block),
             lambda k=k: rcopy(dnp(k), dn_slot(0, far_q, k), x_send.at[2 + k], dn_recv.at[0, k, far_q], peer))
    send_tok = lambda: rcopy(tok_ref, tok_peer, x_send.at[0], x_recv.at[0], peer)
    send(None, send_tok)
    for k in range(PARTS):
        up_forward(f, k, ("r", "l", "y", "p"))
    own_dn = lambda: pltpu.make_async_copy(dnp_ref, dn.at[1, pl.ds(pl.multiple_of(local_f * rd, rd), rd)],
                                           out_sem.at[0])
    pl.when(in_block)(lambda: own_dn().start())

    last = nz - 1
    up_z(1)
    up_y(0)
    for s in range(2, nz):
        up_z(s)
        if s == 2:
            dn_src(0)
        else:
            dn_z(0, s - 2)
        if s == last:
            dn_src(1)
        up_y(s - 1)
    dn_z(0, last - 1)
    up_y(last)
    send_tok().wait_recv()
    norm()
    for s in range(nz):
        up_p(s)
    cuts = [reps * k // nz for k in range(nz + 1)]
    up_dot(cuts[0], cuts[1])
    dn_z(0, last)
    for s in range(1, nz):
        if s < last:
            dn_z(1, s)
        up_dot(cuts[s], cuts[s + 1])
    for s in range(nz):
        dn_y(0, s)
    for s in range(nz):
        dn_p(0, s)
    dn_dot(0, part_out)
    dn_y(1, 0)
    send_part = lambda: rcopy(part_out, part_in, x_send.at[1], x_recv.at[1], peer)
    send(None, send_part)
    dn_z(1, last)
    for s in range(1, nz):
        dn_y(1, s)
    pl.when(in_block)(lambda: own_dn().wait())
    for s in range(nz):
        dn_p(1, s)
    send_part().wait_recv()
    for cond, make in sends:
        guarded(cond, lambda make=make: make().wait_send())


def finish(up, dn, hidden, part_in, up_out, dn_out, mix_out, mix, sems):
    x = lax.axis_index("tp")
    half = dn.shape[2]
    n = sems.shape[1]
    ru, rd = up.shape[0] // n, dn.shape[1] // n
    off = [(1 - x) * half, x * half]
    copies = []
    for k in range(n):
        r = pl.ds(k * ru, ru)
        copies.append(pltpu.make_async_copy(up.at[r], up_out.at[r], sems.at[0, k]))
        r = pl.ds(k * rd, rd)
        for h in range(2):
            cols = pl.ds(pl.multiple_of(off[h], half), half)
            copies.append(pltpu.make_async_copy(dn.at[h, r], dn_out.at[r, cols], sems.at[1 + h, k]))
    for copy in copies:
        copy.start()
    nt = min(256, half)

    @pl.loop(0, half // nt)
    def _(i):
        cols = pl.ds(pl.multiple_of(i * nt, nt), nt)
        own = jnp.dot(hidden[...], dn[1, :, cols], preferred_element_type=F32).astype(BF)
        mix[:, cols] = (own.astype(F32) + part_in[:, cols].astype(F32)).astype(BF)

    last = pltpu.make_async_copy(mix, mix_out, sems.at[3, 0])
    last.start()
    for copy in copies:
        copy.wait()
    last.wait()


def grid_device(nz, tokens, norm_gain, up_trained, down_trained):
    n_fs, n_tp = lax.axis_size("fs"), lax.axis_size("tp")
    ru, width = up_trained.shape
    rd, half = down_trained.shape
    rows = tokens.shape[0]
    d_model, blk = ru * n_fs, n_fs // n_tp
    vmem = pl.BlockSpec(memory_space=pltpu.VMEM)
    hbm = pl.BlockSpec(memory_space=pl.ANY)
    flops = 2 * rows * width * d_model
    held = pl.pallas_call(
        functools.partial(kernel, nz),
        out_shape=(
            jax.ShapeDtypeStruct((d_model, width), BF),
            jax.ShapeDtypeStruct((n_tp, rd * blk, half), BF),
            jax.ShapeDtypeStruct((rows, width), BF),
            jax.ShapeDtypeStruct((rows, half), BF),
        ),
        in_specs=[vmem] * 4,
        out_specs=(vmem,) * 4,
        scratch_shapes=[
            pltpu.VMEM((rd, half), BF),
            pltpu.VMEM((rows, half), BF),
            pltpu.VMEM((n_tp, rows, half), BF),
            pltpu.VMEM((rows, half), BF),
            pltpu.SemaphoreType.DMA((PARTS, n_fs)),
            pltpu.SemaphoreType.DMA((n_tp, PARTS, blk)),
            pltpu.SemaphoreType.DMA((PARTS, n_fs * 4)),
            pltpu.SemaphoreType.DMA((n_tp, PARTS, blk * 4)),
            pltpu.SemaphoreType.DMA((2 + PARTS,)),
            pltpu.SemaphoreType.DMA((2,)),
            pltpu.SemaphoreType.DMA((1,)),
        ],
        compiler_params=pltpu.CompilerParams(
            collective_id=0, has_side_effects=True, vmem_limit_bytes=16 * 2**20
        ),
        cost_estimate=pl.CostEstimate(flops=flops, bytes_accessed=2 * d_model * width * 2, transcendentals=0),
    )(tokens, norm_gain.reshape(1, ru), up_trained, down_trained)
    return pl.pallas_call(
        finish,
        out_shape=(
            jax.ShapeDtypeStruct((d_model, width), BF),
            jax.ShapeDtypeStruct((rd * blk, half * n_tp), BF),
            jax.ShapeDtypeStruct((rows, half), BF),
        ),
        in_specs=[vmem] * 4,
        out_specs=(hbm,) * 3,
        scratch_shapes=[pltpu.VMEM((rows, half), BF), pltpu.SemaphoreType.DMA((4, 8))],
        compiler_params=pltpu.CompilerParams(vmem_limit_bytes=8 * 2**20),
        cost_estimate=pl.CostEstimate(flops=flops, bytes_accessed=2 * d_model * width * 2, transcendentals=0),
    )(*held)


def solution(mesh):
    placed = (P("fs", "tp"), P("fs"), P("fs", "tp"), P("fs", "tp"))
    grid = grid_of(mesh)
    body = plain_device if grid is None else functools.partial(grid_device, grid[0])
    return jax.shard_map(
        body,
        mesh=mesh,
        in_specs=placed,
        out_specs=(P(None, "tp"), P("tp", None), P("fs", "tp")),
        check_vma=False,
    )
```
